32 devices in a mesh: ep: 8 (over z, core), tp: 4 (over y, x).
Axes of the slice: x: 2, y: 2, z: 4, core: 2. Of those that a mesh axis runs over, the one named last changes fastest.
Arguments:
- tokens: bfloat16 [4096, 2048], P(('ep', 'tp')), may hold values from -6 to 6
- norm_gain: float32 [2048], replicated, may hold values from 0.1 to 1.9
- expert_ids: int32 [4096, 2], P(('ep', 'tp')), may hold values from 0 to 7, all different within a row; in each aligned block of 128 rows (0 to 127, 128 to 255, ...) at most 64 rows name the same one
- gate_weights: float32 [4096, 2], P(('ep', 'tp')), may hold values from 0.2 to 1.6
- expert_gate: bfloat16 [8, 512, 2048], P('ep', 'tp'), may hold values from -0.125 to 0.125
- expert_up: bfloat16 [8, 512, 2048], P('ep', 'tp'), may hold values from -0.125 to 0.125
- expert_down: bfloat16 [8, 512, 2048], P('ep', 'tp'), may hold values from -0.25 to 0.25
- shared_gate: bfloat16 [512, 2048], P('tp'), may hold values from -0.125 to 0.125
- shared_up: bfloat16 [512, 2048], P('tp'), may hold values from -0.125 to 0.125
- shared_down: bfloat16 [512, 2048], P('tp'), may hold values from -0.25 to 0.25
Outputs:
- mixed: bfloat16 [4096, 2048], P(('ep', 'tp'))
The draws below stay inside these ranges and needn't reach their ends.
Inputs may be any that keep to these rules, and one draw needn't show every extreme that they name: `expert_ids`: each row names 2 different experts. Within the rows of one device no expert is named by more than 64 rows, and in every draw some expert is named by exactly 64 rows of some device.
All inputs are finite; a program needn't handle non-finite values.
Results may differ from the reference program's by a relative error of at most 0.0068.
Values may be sent and summed in bfloat16 or wider, within the bound.
A program may use at most 64 MiB of HBM per device.

```python
import math
import jax
import jax.numpy as jnp
import numpy as np
from jax import lax

D = 2048
FF = 512
SFF = 512
K = 2
TOK_DEV = 128
EXPERTS = 8
CAP = 64
TOKENS = 4096


def block_levels(rng, shape, shards, smallest, largest):
    gain = 1.0
    for dim, parts in shards:
        draws = jax.random.uniform(jax.random.fold_in(jax.random.fold_in(rng, 6), dim), (parts,), jnp.float32, smallest / len(shards), largest / len(shards))
        gain = gain * jnp.repeat(jnp.exp(draws), shape[dim] // parts).reshape((-1,) + (1,) * (len(shape) - 1 - dim))
    return gain


def deal_out(own_key, own, number, rows, amount, top, limit, skew):
    sequence = jax.random.permutation(own_key, amount)
    packed, common = shares(amount, rows * top, limit, skew, True), shares(amount, rows * top, limit, skew, False)
    places = jnp.arange(amount)

    def named(tallies, turn):
        used = int((tallies > 0).sum())
        fixed = max(1, used // 4)
        shifted = fixed + (places - fixed + turn * (used - fixed)) % max(1, amount - fixed)
        return jnp.zeros((amount,), jnp.int32).at[sequence[jnp.where(places < fixed, places, shifted)]].set(jnp.asarray(tallies, jnp.int32))

    tallies = jnp.where(number % 4 == 0, named(packed, number // 4), named(common, number - number // 4 - 1))
    mixed = jax.random.permutation(jax.random.fold_in(own, 3), amount)
    giver, taker = mixed[0:amount // 2 * 2:2], mixed[1:amount // 2 * 2:2]
    slack = jnp.minimum(tallies[giver] - 1, limit - tallies[taker]) // 2
    slack = jnp.where((giver == sequence[0]) | (taker == sequence[0]) | (tallies[taker] == 0), 0, jnp.maximum(slack, 0))
    shifted = jax.random.randint(jax.random.fold_in(own, 4), (amount // 2,), 0, 1 << 20) % (slack + 1)
    tallies = tallies.at[giver].add(-shifted).at[taker].add(shifted)
    members = jnp.searchsorted(jnp.cumsum(tallies), jnp.arange(rows * top), side="right").astype(jnp.int32)
    listing = members.reshape(top, rows).T
    listing = listing[jax.random.permutation(jax.random.fold_in(own, 1), rows)]
    turn = jax.random.randint(jax.random.fold_in(own, 2), (rows, 1), 0, top)
    return jnp.take_along_axis(listing, (jnp.arange(top)[None, :] + turn) % top, axis=1)


def shares(amount, total, bound, lean, full):
    portions = [(1 << 20) // math.isqrt(standing ** lean) + 1 for standing in range(1, amount + 1)]
    largest = bound if full else min(bound, max(-(-total // amount), total * portions[0] // sum(portions)))
    least = 1 if total - largest >= amount - 1 else 0
    counts, rest = [largest] + [least] * (amount - 1), total - largest - least * (amount - 1)
    while rest > 0:
        free = [i for i in range(1, amount) if counts[i] < largest] or [i for i in range(1, amount) if counts[i] < bound]
        mass, left = sum([portions[i] for i in free]), rest
        for i in free:
            addition = min(bound - counts[i], max(1, left * portions[i] // mass), rest)
            counts[i] = counts[i] + addition
            rest = rest - addition
    return np.array(counts)


def normal_values(rng, extent, spread, reach, pieces=(), held_as=jnp.bfloat16):
    values = spread * jax.random.normal(rng, extent, jnp.float32)
    if pieces:
        values = values * block_levels(rng, extent, pieces, -0.22, 0.18)
    return jnp.clip(values, -reach, reach).astype(held_as)


def setup_inputs(seed: int = 0) -> dict:
    seeds = jax.random.split(jax.random.key(seed), 11)
    tokens = normal_values(seeds[0], (TOKENS, D), 1.0, 6.0, ((0, 32),))
    norm_gain = jnp.clip(1.0 + 0.18 * jax.random.normal(seeds[1], (D,), jnp.float32), 0.1, 1.9)
    expert_ids_keys = jax.random.split(jax.random.fold_in(seeds[2], 1), TOKENS // TOK_DEV)
    expert_ids_turns = jax.random.permutation(jax.random.fold_in(seeds[2], 3), TOKENS // TOK_DEV)
    expert_ids = jax.vmap(lambda own, number: deal_out(jax.random.fold_in(seeds[2], 2), own, number, TOK_DEV, EXPERTS, K, CAP, 2))(expert_ids_keys, expert_ids_turns).reshape((TOKENS, K))
    gate_weights = jnp.clip(0.2 + 1.4 * jax.random.uniform(seeds[3], (TOKENS, K), jnp.float32) ** block_levels(seeds[3], (TOKENS, K), ((0, 32),), -0.2, 0.2), 0.2, 1.6)
    expert_gate = normal_values(seeds[4], (EXPERTS, FF, D), D ** -0.5, 0.125, ((0, 8), (1, 4)))
    expert_up = normal_values(seeds[5], (EXPERTS, FF, D), D ** -0.5, 0.125, ((0, 8), (1, 4)))
    expert_down = normal_values(seeds[6], (EXPERTS, FF, D), FF ** -0.5, 0.25, ((0, 8), (1, 4)))
    shared_gate = normal_values(seeds[7], (SFF, D), D ** -0.5, 0.125, ((0, 4),))
    shared_up = normal_values(seeds[8], (SFF, D), D ** -0.5, 0.125, ((0, 4),))
    shared_down = normal_values(seeds[9], (SFF, D), SFF ** -0.5, 0.25, ((0, 4),))
    return {"tokens": tokens, "norm_gain": norm_gain, "expert_ids": expert_ids, "gate_weights": gate_weights, "expert_gate": expert_gate, "expert_up": expert_up, "expert_down": expert_down, "shared_gate": shared_gate, "shared_up": shared_up, "shared_down": shared_down}


EPS = 1e-06

def against(rows, weight):
    return jnp.dot(rows, weight.T, preferred_element_type=jnp.float32)

def reference(tokens, norm_gain, expert_ids, gate_weights, expert_gate, expert_up, expert_down, shared_gate, shared_up, shared_down):
    tok = tokens.astype(jnp.float32)
    normed = (tok * lax.rsqrt(lax.optimization_barrier(jnp.mean(tok * tok, axis=-1, keepdims=True)) + EPS) * norm_gain).astype(jnp.bfloat16)
    most_rows = TOKENS // TOK_DEV * CAP
    order = jnp.arange(TOKENS, dtype=jnp.int32)

    def one_expert(index, routed):
        named = expert_ids == index
        member = jnp.any(named, axis=1).astype(jnp.int32)
        weight_row = lax.optimization_barrier(jnp.sum(jnp.where(named, gate_weights, 0.0), axis=1))
        place = (jnp.cumsum(member) - member).astype(jnp.int32)
        place = jnp.where(member > 0, place, most_rows).astype(jnp.int32)
        table = jnp.full((most_rows,), TOKENS, jnp.int32).at[place].set(order, mode='drop')
        rows = jnp.take(normed, table, axis=0, mode='fill', fill_value=0)
        scale = jnp.take(weight_row, table, axis=0, mode='fill', fill_value=0)
        gate = lax.dynamic_index_in_dim(expert_gate, index, 0, keepdims=False)
        up = lax.dynamic_index_in_dim(expert_up, index, 0, keepdims=False)
        down = lax.dynamic_index_in_dim(expert_down, index, 0, keepdims=False)
        hidden = (jax.nn.silu(against(rows, gate)) * against(rows, up)).astype(jnp.bfloat16)
        result = jnp.dot(hidden, down, preferred_element_type=jnp.float32).astype(jnp.bfloat16)
        return routed.at[table].add(scale[:, None] * result.astype(jnp.float32), mode='drop')
    routed = lax.fori_loop(0, EXPERTS, one_expert, jnp.zeros((TOKENS, D), jnp.float32))
    shared_hidden = (jax.nn.silu(against(normed, shared_gate)) * against(normed, shared_up)).astype(jnp.bfloat16)
    shared = jnp.dot(shared_hidden, shared_down, preferred_element_type=jnp.float32)
    return (routed + shared).astype(jnp.bfloat16)
```

```python
import functools
import math

import jax
import jax.numpy as jnp
from jax import lax
from jax.experimental import pallas as pl
from jax.experimental.pallas import tpu as pltpu
from jax.sharding import PartitionSpec as P

EPS = 1e-06
MESH = pl.DeviceIdType.MESH
NT = (((1,), (1,)), ((), ()))
F32 = jnp.float32
BF16 = jnp.bfloat16
CHUNKS = 8
SPIECES = 2
REACH = 2


def remote(src, dst, send, recv, where):
    return pltpu.make_async_remote_copy(
        src_ref=src, dst_ref=dst, send_sem=send, recv_sem=recv, device_id=where, device_id_type=MESH
    )


def runs_of(slots):
    out = []
    for s in slots:
        if out and out[-1][1] == s:
            out[-1][1] = s + 1
        else:
            out.append([s, s + 1])
    return out


def kernel(
    ep, tp, xs, ys, nsh,
    tok_ref, gain_ref, ids_ref, gw_ref, eg, eu, ed, sg, su, sd, out_ref,
    tokv, act, wsend, wrecv, wcol, wts, swts, hid, shid, acc, fin, ring,
    lt, lw, ls, s1, r1, s2, r2, s3, r3, st, rt, sw, rw, sc, rc,
):
    e = lax.axis_index("ep")
    t = lax.axis_index("tp")
    y, x = t // xs, t % xs
    z, core = e // 2, e % 2
    nz = ep // 2
    partner = e + 1 - 2 * core
    rows, d_model = tok_ref.shape
    own_rows = eg.shape[0]
    srows = swts.shape[3]
    piece = d_model // CHUNKS
    spiece = d_model // SPIECES
    half_rows = rows // 2
    z0 = (nz - nsh) // 2
    last = 2 + CHUNKS
    sdown = last + 2
    shares = (z >= z0) & (z < z0 + nsh)

    def at(dy, dx):
        return lax.rem(y + dy, ys) * xs + lax.rem(x + dx, xs)

    def slot(dy, dx):
        return (dy % ys) * xs + dx % xs

    row_off = [(0, i) for i in range(1, xs)]
    col_off = [(i, 0) for i in range(1, ys)]
    near_off = row_off + col_off
    diag_off = [(i, j) for i in range(1, ys) for j in range(1, xs)]
    near_slots = sorted([0] + [slot(*o) for o in near_off])
    diag_slots = sorted(slot(*o) for o in diag_off)

    mine = pl.ds(pl.multiple_of(((z - z0) * 2 + core) * srows, srows), srows)
    loads = [
        pltpu.make_async_copy(tok_ref, tokv, lt.at[0]),
        pltpu.make_async_copy(eg, wts.at[0, core, 0], lw.at[0]),
        pltpu.make_async_copy(eu, wts.at[1, core, 0], lw.at[1]),
        pltpu.make_async_copy(ed, wts.at[2, core, 0], lw.at[2]),
    ]
    for c in loads:
        c.start()
    sloads = [pltpu.make_async_copy(r.at[mine], swts.at[i, core, 0], ls.at[i]) for i, r in enumerate((sg, su, sd))]

    @pl.when(shares)
    def _():
        for c in sloads:
            c.start()

    barrier = pltpu.get_barrier_semaphore()
    for o in near_off:
        pl.semaphore_signal(barrier, inc=1, device_id={"tp": at(*o)}, device_id_type=MESH)
    for i in range(1, nz):
        pl.semaphore_signal(barrier, inc=1, device_id={"ep": lax.rem(e + 2 * i, ep)}, device_id_type=MESH)
    pl.semaphore_signal(barrier, inc=1, device_id={"ep": partner}, device_id_type=MESH)

    chosen = ids_ref.shape[0]
    sub = lax.broadcasted_iota(jnp.int32, (8, rows), 0)
    for p in range(nz):
        label = sub + 2 * p
        total = jnp.zeros((8, rows), F32)
        for k in range(chosen):
            total = total + jnp.where(ids_ref[k : k + 1, :] == label, gw_ref[k : k + 1, :], 0.0)
        wsend[p] = total
    loads[0].wait()
    tok = tokv[...].astype(F32)
    nrm = tok * lax.rsqrt(jnp.mean(tok * tok, axis=-1, keepdims=True) + EPS) * gain_ref[...]
    act[z] = nrm.astype(BF16)
    for c in loads[1:]:
        c.wait()

    @pl.when(shares)
    def _():
        for c in sloads:
            c.wait()

    pl.semaphore_wait(barrier, len(near_off) + nz)

    sends = []
    ssends = []

    def columns(a):
        if 2 <= a < last:
            return (a - 2) * piece, piece
        if a >= sdown:
            return (a - sdown) * spiece, spiece
        return 0, d_model

    def view(a, k, s, start, size):
        cols = pl.ds(start, size)
        if a < last:
            return wts.at[min(a, 2), k, s, :, cols]
        return swts.at[min(a - last, 2), k, s, :, cols]

    def block(a, k, s):
        return view(a, k, s, *columns(a))

    def part(a, s, h):
        start, size = columns(a)
        return view(a, core, s, start + h * (size // 2), size // 2)

    def keep(a, *parts):
        make = functools.partial(copy_of, a, *parts)
        (sends if a < last else ssends).append(make)
        make().start()

    def copy_of(a, kind, *where):
        if kind == "over":
            (s,) = where
            return remote(block(a, core, s), block(a, core, s), s3.at[a, s], r3.at[a, s], {"ep": partner})
        if kind == "first":
            j, (dy, dx) = where
            to = slot(-dy, -dx)
            return remote(block(a, core, 0), block(a, core, to), s1.at[a, j], r1.at[a, to], {"tp": at(dy, dx)})
        h, i, j, (oy, ox), (py, px) = where
        to = slot(oy - py, ox - px)
        return remote(part(a, slot(oy, ox), h), part(a, to, h), s2.at[a, h, i, j], r2.at[a, h, to], {"tp": at(py, px)})

    def over(a, s):
        keep(a, "over", s)

    def first(a):
        for j, o in enumerate(near_off):
            keep(a, "first", j, o)

    def first_done(a):
        for o in near_off:
            s = slot(*o)
            remote(block(a, core, s), block(a, core, s), s1.at[a, 0], r1.at[a, s], {"tp": t}).wait_recv()

    def second(a):
        for h, (owners, peers) in enumerate(((col_off, row_off), (row_off, col_off))):
            for i, o in enumerate(owners):
                for j, p in enumerate(peers):
                    keep(a, "second", h, i, j, o, p)

    def second_done(a):
        for s in diag_slots:
            for h in range(2):
                remote(part(a, s, h), part(a, s, h), s2.at[a, h, 0, 0], r2.at[a, h, s], {"tp": t}).wait_recv()

    def over_done(a, slots):
        for s in slots:
            b = block(a, 1 - core, s)
            remote(b, b, s3.at[a, s], r3.at[a, s], {"ep": partner}).wait_recv()

    def relay(a):
        first_done(a)
        second(a)
        for s in near_slots[1:]:
            over(a, s)

    def finish(a):
        second_done(a)
        for s in diag_slots:
            over(a, s)

    def hop(src, h, sign):
        ref = act.at[src, pl.ds(h * half_rows, half_rows), :]
        return remote(ref, ref, st.at[0 if sign > 0 else 1, src, h], rt.at[src, h], {"ep": e + 2 * sign})

    def travel(step, h, act_on):
        for sign in (1, -1):
            src = z - sign * step
            there = (src >= 0) if sign > 0 else (src < nz)
            on = (z + 1 < nz) if sign > 0 else (z > 0)
            act_on(src, h, sign, there, on)

    def pass_on(src, h, sign, there, on):
        @pl.when(there)
        def _():
            hop(src, h, sign).wait_recv()

            @pl.when(on)
            def _():
                hop(src, h, sign).start()

    first(0)
    for h in range(2):
        for sign in (1, -1):
            on = (z + 1 < nz) if sign > 0 else (z > 0)

            @pl.when(on)
            def _():
                hop(z, h, sign).start()

    over(0, 0)
    over(1, 0)
    first(1)
    for i in range(1, nz):
        p = lax.rem(z + i, nz)
        c = remote(wsend.at[p], wrecv.at[z], sw.at[i], rw.at[z], {"ep": 2 * p + core})
        c.start()
    wrecv[z] = wsend[z]
    for n in range(CHUNKS):
        over(2 + n, 0)

    for i in range(1, nz):
        p = lax.rem(z + i, nz)
        remote(wrecv.at[p], wrecv.at[p], sw.at[0], rw.at[p], {"ep": e}).wait_recv()

    def turn(p, carry):
        wcol[p] = wrecv[p].T
        return carry

    lax.fori_loop(0, nz, turn, 0)

    def ffn(p, planes, groups):
        m = planes * rows
        held = act[pl.ds(p, planes)].reshape(m, d_model)
        scale = wcol[pl.ds(p, planes)].reshape(m, 8)
        for k in range(2):
            for lo, hi in groups:
                width = (hi - lo) * own_rows
                gate = lax.dot_general(held, wts[0, k, lo:hi].reshape(width, d_model), NT, preferred_element_type=F32)
                up = lax.dot_general(held, wts[1, k, lo:hi].reshape(width, d_model), NT, preferred_element_type=F32)
                val = gate * (1.0 / (1.0 + jnp.exp(-gate))) * up * scale[:, k : k + 1]
                base = (k * tp + lo) * own_rows
                hid[pl.ds(p, planes), :, base : base + width] = val.astype(BF16).reshape(planes, rows, width)

    def ffn_loop(lo, hi, groups):
        def step(p, carry):
            ffn(p, 1, groups)
            return carry

        lax.fori_loop(lo, hi, step, 0)

    staged = own_rows % 128 == 0
    pack = math.gcd(nz, 4)

    for h in range(2):
        travel(1, h, pass_on)
    relay(0)
    for h in range(2):
        if nz > 2:
            travel(2, h, pass_on)
    relay(1)

    @pl.when(shares)
    def _():
        first(last)
        first(last + 1)

    first(2)
    first(3)
    over_done(0, near_slots)
    over_done(1, near_slots)
    low = jnp.maximum(z - REACH, 0)
    high = jnp.minimum(z + REACH + 1, nz)
    if staged:
        ffn_loop(low, high, runs_of(near_slots))
    if nz > 3:
        travel(3, 0, pass_on)
    finish(0)
    if nz > 3:
        travel(3, 1, pass_on)
    for step in range(4, nz):
        for h in range(2):
            travel(step, h, pass_on)
    if staged:
        ffn_loop(0, low, runs_of(near_slots))
        ffn_loop(high, nz, runs_of(near_slots))
    finish(1)

    @pl.when(shares)
    def _():
        relay(last)
        relay(last + 1)
        over(last, 0)
        over(last + 1, 0)
        for n in range(SPIECES):
            over(sdown + n, 0)
        first(sdown)

    relay(2)
    first(4)
    over_done(0, diag_slots)
    over_done(1, diag_slots)
    tail = diag_slots if staged else list(range(tp))

    def late(i, carry):
        ffn(i * pack, pack, runs_of(tail))
        return carry

    lax.fori_loop(0, nz // pack, late, 0)
    all_slots = near_slots + diag_slots

    @pl.when(shares)
    def _():
        finish(last)
        finish(last + 1)
        relay(sdown)
        for n in range(1, SPIECES):
            first(sdown + n)
        over_done(last, all_slots)
        over_done(last + 1, all_slots)
        sall = 2 * tp * srows

        def shared(i, carry):
            held = act[pl.ds(i * pack, pack)].reshape(pack * rows, d_model)
            gate = lax.dot_general(held, swts[0].reshape(sall, d_model), NT, preferred_element_type=F32)
            up = lax.dot_general(held, swts[1].reshape(sall, d_model), NT, preferred_element_type=F32)
            val = gate * (1.0 / (1.0 + jnp.exp(-gate))) * up
            shid[pl.ds(i * pack, pack)] = val.astype(BF16).reshape(pack, rows, sall)
            return carry

        lax.fori_loop(0, nz // pack, shared, 0)

    def link(n, d, sign, j):
        cols = pl.ds(n * piece, piece)
        to = nz if (sign < 0 and j == 1) else d
        return remote(ring.at[d, :, cols], ring.at[to, :, cols], sc.at[n, d], rc.at[n, to], {"ep": e + 2 * sign})

    def landed(n, s):
        ref = ring.at[s, :, pl.ds(n * piece, piece)]
        remote(ref, ref, sc.at[n, 0], rc.at[n, s], {"ep": e}).wait_recv()

    def each_link(run):
        for j in range(nz - 1, 0, -1):
            for sign in (1, -1):
                d = z + sign * j
                there = (d < nz) if sign > 0 else (d >= 0)
                fed = (z > 0) if sign > 0 else (z < nz - 1)

                @pl.when(there)
                def _():
                    run(d, sign, j, fed)

    for n in range(CHUNKS):
        lo, hi = n * piece, (n + 1) * piece
        finish(n + 2)
        over_done(n + 2, all_slots)
        if n % (CHUNKS // SPIECES) == 0:
            q = n // (CHUNKS // SPIECES)

            @pl.when(shares)
            def _():
                if q > 0:
                    relay(sdown + q)
                finish(sdown + q)
                over_done(sdown + q, all_slots)

        def down(i, carry):
            left = hid[pl.ds(i * pack, pack)].reshape(pack * rows, 2 * tp * own_rows)
            right = wts[2, :, :, :, lo:hi].reshape(2 * tp * own_rows, piece)
            o = jnp.dot(left, right, preferred_element_type=F32)
            acc[pl.ds(i * pack, pack)] = o.reshape(pack, rows, piece)

            @pl.when(shares)
            def _():
                more = jnp.dot(
                    shid[pl.ds(i * pack, pack)].reshape(pack * rows, 2 * tp * srows),
                    swts[2, :, :, :, lo:hi].reshape(2 * tp * srows, piece),
                    preferred_element_type=F32,
                )
                acc[pl.ds(i * pack, pack)] += more.reshape(pack, rows, piece)

            return carry

        lax.fori_loop(0, nz // pack, down, 0)
        fin[:, lo:hi] = acc[z]

        if n + 3 < last:
            relay(n + 3)
        if n + 5 < last:
            first(n + 5)

        def run(d, sign, j, fed):
            @pl.when(fed)
            def _():
                landed(n, d)
                ring[d, :, lo:hi] = (acc[d] + ring[d, :, lo:hi].astype(F32)).astype(BF16)

            @pl.when(jnp.logical_not(fed))
            def _():
                ring[d, :, lo:hi] = acc[d].astype(BF16)

            link(n, d, sign, j).start()

        each_link(run)

    for n in range(CHUNKS):
        lo, hi = n * piece, (n + 1) * piece

        @pl.when(z > 0)
        def _():
            landed(n, z)
            fin[:, lo:hi] += ring[z, :, lo:hi].astype(F32)

        @pl.when(z < nz - 1)
        def _():
            landed(n, nz)
            fin[:, lo:hi] += ring[nz, :, lo:hi].astype(F32)

        out_ref[:, lo:hi] = fin[:, lo:hi].astype(BF16)

    for i in range(1, nz):
        p = lax.rem(z + i, nz)
        remote(wsend.at[p], wrecv.at[z], sw.at[i], rw.at[z], {"ep": 2 * p + core}).wait_send()
    for make in sends:
        make().wait_send()

    @pl.when(shares)
    def _():
        for make in ssends:
            make().wait_send()

    for n in range(CHUNKS):
        each_link(lambda d, sign, j, fed: link(n, d, sign, j).wait_send())

    for h in range(2):
        for sign in (1, -1):
            on = (z + 1 < nz) if sign > 0 else (z > 0)

            @pl.when(on)
            def _():
                hop(z, h, sign).wait_send()

        for step in range(1, nz):

            def sent(src, h, sign, there, on):
                @pl.when(there & on)
                def _():
                    hop(src, h, sign).wait_send()

            travel(step, h, sent)


def body(ep, tp, tokens, norm_gain, expert_ids, gate_weights, eg, eu, ed, sg, su, sd):
    rows, d_model = tokens.shape
    side = math.isqrt(tp)
    xs = side if side * side == tp else tp
    ys = tp // xs
    nz = ep // 2
    own_rows = eg.shape[1]
    nsh = max(1, min(sg.shape[0] // 32, nz - 2))
    srows = sg.shape[0] // (2 * nsh)
    near = xs + ys - 2
    far = max(xs, ys)
    moves = 2 + CHUNKS + 2 + SPIECES
    dma = pltpu.SemaphoreType.DMA
    vm = pl.BlockSpec(memory_space=pltpu.VMEM)
    hbm = pl.BlockSpec(memory_space=pl.ANY)
    return pl.pallas_call(
        functools.partial(kernel, ep, tp, xs, ys, nsh),
        out_shape=jax.ShapeDtypeStruct((rows, d_model), BF16),
        in_specs=[hbm, vm, vm, vm] + [hbm] * 6,
        out_specs=vm,
        scratch_shapes=[
            pltpu.VMEM((rows, d_model), BF16),
            pltpu.VMEM((nz, rows, d_model), BF16),
            pltpu.VMEM((nz, 8, rows), F32),
            pltpu.VMEM((nz, 8, rows), F32),
            pltpu.VMEM((nz, rows, 8), F32),
            pltpu.VMEM((3, 2, tp, own_rows, d_model), BF16),
            pltpu.VMEM((3, 2, tp, srows, d_model), BF16),
            pltpu.VMEM((nz, rows, 2 * tp * own_rows), BF16),
            pltpu.VMEM((nz, rows, 2 * tp * srows), BF16),
            pltpu.VMEM((nz, rows, d_model // CHUNKS), F32),
            pltpu.VMEM((rows, d_model), F32),
            pltpu.VMEM((nz + 1, rows, d_model), BF16),
            dma((1,)),
            dma((3,)),
            dma((3,)),
            dma((moves, near)),
            dma((moves, tp)),
            dma((moves, 2, far, far)),
            dma((moves, 2, tp)),
            dma((moves, tp)),
            dma((moves, tp)),
            dma((2, nz, 2)),
            dma((nz, 2)),
            dma((nz,)),
            dma((nz,)),
            dma((CHUNKS, nz)),
            dma((CHUNKS, nz + 1)),
        ],
        compiler_params=pltpu.CompilerParams(
            collective_id=0, has_side_effects=True, vmem_limit_bytes=62 * 1024 * 1024
        ),
        name="moe",
    )(tokens, norm_gain.reshape(1, d_model), expert_ids.T, gate_weights.T, eg[0], eu[0], ed[0], sg, su, sd)


def solution(mesh):
    in_specs = (
        P(("ep", "tp"), None),
        P(),
        P(("ep", "tp"), None),
        P(("ep", "tp"), None),
        P("ep", "tp", None),
        P("ep", "tp", None),
        P("ep", "tp", None),
        P("tp", None),
        P("tp", None),
        P("tp", None),
    )
    out_specs = P(("ep", "tp"), None)
    return jax.shard_map(
        functools.partial(body, mesh.shape["ep"], mesh.shape["tp"]),
        mesh=mesh, in_specs=in_specs, out_specs=out_specs, check_vma=False,
    )
```

```python
import functools
import math

import jax
import jax.numpy as jnp
from jax import lax
from jax.experimental import pallas as pl
from jax.experimental.pallas import tpu as pltpu
from jax.sharding import PartitionSpec as P

EPS = 1e-06
MESH = pl.DeviceIdType.MESH
NT = (((1,), (1,)), ((), ()))
F32 = jnp.float32
BF16 = jnp.bfloat16
CHUNKS = 8
SPIECES = 2
REACH = 2
PIECES = ((0, 1), (1, 1), (2, 2), (4, 2), (6, 2))


def remote(src, dst, send, recv, where):
    return pltpu.make_async_remote_copy(
        src_ref=src, dst_ref=dst, send_sem=send, recv_sem=recv, device_id=where, device_id_type=MESH
    )


def runs_of(slots):
    out = []
    for s in slots:
        if out and out[-1][1] == s:
            out[-1][1] = s + 1
        else:
            out.append([s, s + 1])
    return out


def kernel(
    ep, tp, xs, ys, nsh,
    tok_ref, gain_ref, ids_ref, gw_ref, eg, eu, ed, sg, su, sd, out_ref,
    tokv, act, wtab, wcol, wts, swts, gbuf, hid, shid, acc, fin, ring,
    ld, sx, r1, r2, r3, r4, st, rt, sw, rw, sc, rc,
):
    e = lax.axis_index("ep")
    t = lax.axis_index("tp")
    y, x = t // xs, t % xs
    z, core = e // 2, e % 2
    nz = ep // 2
    partner = e + 1 - 2 * core
    rows, d_model = tok_ref.shape
    own_rows = eg.shape[0]
    srows = swts.shape[3]
    piece = d_model // CHUNKS
    spiece = d_model // SPIECES
    half_rows = rows // 2
    z0 = (nz - nsh) // 2
    parts = len(PIECES)
    last = 2 + parts
    sdown = last + 1
    shares = (z >= z0) & (z < z0 + nsh)

    def at(dy, dx):
        return lax.rem(y + dy, ys) * xs + lax.rem(x + dx, xs)

    def slot(dy, dx):
        return (dy % ys) * xs + dx % xs

    row_off = [(0, i) for i in range(1, xs)]
    col_off = [(i, 0) for i in range(1, ys)]
    near_off = row_off + col_off
    near_slots = sorted([0] + [slot(*o) for o in near_off])
    diag_slots = [s for s in range(tp) if s not in near_slots]
    near, ndiag = len(near_off), len(diag_slots)

    mine = pl.ds(pl.multiple_of(((z - z0) * 2 + core) * srows, srows), srows)
    loads = [
        pltpu.make_async_copy(tok_ref, tokv, ld.at[0]),
        pltpu.make_async_copy(eg, wts.at[0, 0, core], ld.at[1]),
        pltpu.make_async_copy(eu, wts.at[1, 0, core], ld.at[2]),
        pltpu.make_async_copy(ed, wts.at[2, 0, core], ld.at[3]),
    ]
    for c in loads:
        c.start()
    sloads = [pltpu.make_async_copy(r.at[mine], swts.at[i, 0, core], ld.at[4 + i]) for i, r in enumerate((sg, su, sd))]

    @pl.when(shares)
    def _():
        for c in sloads:
            c.start()

    barrier = pltpu.get_barrier_semaphore()
    for o in near_off:
        pl.semaphore_signal(barrier, inc=1, device_id={"tp": at(*o)}, device_id_type=MESH)
    pl.semaphore_signal(barrier, inc=1, device_id={"ep": partner}, device_id_type=MESH)
    for sign in (1, -1):
        on = (z + 1 < nz) if sign > 0 else (z > 0)

        @pl.when(on)
        def _():
            pl.semaphore_signal(barrier, inc=1, device_id={"ep": e + 2 * sign}, device_id_type=MESH)

    chosen = ids_ref.shape[0]
    label = lax.broadcasted_iota(jnp.int32, wtab.shape[1:], 0)
    total = jnp.zeros(wtab.shape[1:], F32)
    for k in range(chosen):
        total = total + jnp.where(ids_ref[k : k + 1, :] == label, gw_ref[k : k + 1, :], 0.0)
    wtab[z] = total
    loads[0].wait()
    tok = tokv[...].astype(F32)
    nrm = tok * lax.rsqrt(jnp.mean(tok * tok, axis=-1, keepdims=True) + EPS) * gain_ref[...]
    act[z] = nrm.astype(BF16)
    for c in loads[1:]:
        c.wait()

    @pl.when(shares)
    def _():
        for c in sloads:
            c.wait()

    pl.semaphore_wait(barrier, near + 1 + (z > 0).astype(jnp.int32) + (z < nz - 1).astype(jnp.int32))

    def columns(a):
        if 2 <= a < last:
            lo, count = PIECES[a - 2]
            return lo * piece, count * piece
        if a >= sdown:
            return (a - sdown) * spiece, spiece
        return 0, d_model

    def view(a, s, k, start, size):
        cols = pl.ds(start, size)
        if a < last:
            return wts.at[min(a, 2), s, k, :, cols]
        if a == last:
            return swts.at[pl.ds(0, 2), s, k, :, cols]
        return swts.at[2, s, k, :, cols]

    def block(a, s, k):
        return view(a, s, k, *columns(a))

    def part(a, s, h):
        start, size = columns(a)
        return view(a, s, core, start + h * (size // 2), size // 2)

    def first(a):
        for dy, dx in near_off:
            to = slot(-dy, -dx)
            remote(block(a, 0, core), block(a, to, core), sx.at[int(a >= last), 0], r1.at[a], {"tp": at(dy, dx)}).start()

    def second(a):
        for h, (owners, peers) in enumerate(((col_off, row_off), (row_off, col_off))):
            for oy, ox in owners:
                for py, px in peers:
                    to = slot(oy - py, ox - px)
                    remote(part(a, slot(oy, ox), h), part(a, to, h), sx.at[int(a >= last), 1], r2.at[a], {"tp": at(py, px)}).start()

    def over(a, slots, sem):
        for s in slots:
            b = block(a, s, core)
            remote(b, b, sx.at[int(a >= last), 2], sem, {"ep": partner}).start()

    def arrive(ref, sem):
        remote(ref, ref, sx.at[0, 0], sem, {"ep": partner}).wait_recv()

    def relay(a):
        arrive(block(a, pl.ds(0, near), core), r1.at[a])
        second(a)
        over(a, near_slots[1:], r3.at[a, 0])

    def finish(a):
        arrive(block(a, pl.ds(0, ndiag), core), r2.at[a])
        over(a, diag_slots, r3.at[a, 1])

    def near_over(a):
        arrive(block(a, pl.ds(0, near), 1 - core), r3.at[a, 0])

    def diag_over(a):
        arrive(block(a, pl.ds(0, ndiag), 1 - core), r3.at[a, 1])

    def token_copy(src, h, sign, sem):
        ref = act.at[src, pl.ds(h * half_rows, half_rows), :]
        return remote(ref, ref, st.at[sem], rt.at[src, h], {"ep": e + 2 * sign})

    def table_copy(src, sign, sem):
        return remote(wtab.at[src], wtab.at[src], sw.at[sem], rw.at[src], {"ep": e + 2 * sign})

    def travel(step, h):
        for sign in (1, -1):
            src = z - sign * step
            there = (src >= 0) if sign > 0 else (src < nz)
            on = (z + 1 < nz) if sign > 0 else (z > 0)

            @pl.when(there)
            def _():
                if h == 0:
                    table_copy(src, sign, src).wait_recv()
                    wcol[src] = wtab[src].T

                    @pl.when(on)
                    def _():
                        table_copy(src, sign, src).start()

                token_copy(src, h, sign, src).wait_recv()

                @pl.when(on)
                def _():
                    token_copy(src, h, sign, src).start()

    def own_tokens(run):
        for sign in (1, -1):
            on = (z + 1 < nz) if sign > 0 else (z > 0)
            sem = z if sign > 0 else nz

            @pl.when(on)
            def _():
                run(sign, sem)

    own_tokens(lambda sign, sem: table_copy(z, sign, sem).start())
    first(0)
    for h in range(2):
        own_tokens(lambda sign, sem: token_copy(z, h, sign, sem).start())
    over(0, [0], r4.at[0])
    over(1, [0], r4.at[0])
    first(1)
    first(2)

    @pl.when(shares)
    def _():
        first(last)
        over(last, [0], r4.at[2])
        own = swts.at[2, 0, core]
        remote(own, own, sx.at[1, 2], r4.at[3], {"ep": partner}).start()

    own = wts.at[2, 0, core]
    remote(own, own, sx.at[0, 2], r4.at[1], {"ep": partner}).start()
    wcol[z] = wtab[z].T

    lanes = lax.broadcasted_iota(jnp.int32, (1, wcol.shape[2]), 1)

    def weighted(gate, up, p, planes):
        m, width = gate.shape
        col = wcol[pl.ds(p, planes)].reshape(m, wcol.shape[2])
        pair = [jnp.sum(jnp.where(lanes == 2 * z + k, col, 0.0), axis=1, keepdims=True) for k in range(2)]
        which = lax.broadcasted_iota(jnp.int32, (1, width), 1) // own_rows % 2
        scale = jnp.where(which == 0, pair[0], pair[1])
        val = gate * (1.0 / (1.0 + jnp.exp(-gate))) * up * scale
        return val.astype(BF16).reshape(planes, rows, width)

    def project(a, p, planes, lo, hi):
        held = act[pl.ds(p, planes)].reshape(planes * rows, d_model)
        weight = wts[a, lo:hi].reshape((hi - lo) * 2 * own_rows, d_model)
        return lax.dot_general(held, weight, NT, preferred_element_type=F32)

    def ffn(p, planes, groups):
        for lo, hi in groups:
            val = weighted(project(0, p, planes, lo, hi), project(1, p, planes, lo, hi), p, planes)
            hid[pl.ds(p, planes), :, lo * 2 * own_rows : hi * 2 * own_rows] = val

    def ffn_loop(lo, hi, groups):
        def step(p, carry):
            ffn(p, 1, groups)
            return carry

        lax.fori_loop(lo, hi, step, 0)

    staged = own_rows % 128 == 0 and len(runs_of(near_slots)) == 1
    pack = math.gcd(nz, 4)
    low = jnp.maximum(z - REACH, 0)
    high = jnp.minimum(z + REACH + 1, nz)
    dlo, dhi = min(diag_slots), max(diag_slots) + 1

    for h in range(2):
        travel(1, h)
    relay(0)
    if nz > 2:
        for h in range(2):
            travel(2, h)
    relay(1)
    relay(2)

    @pl.when(shares)
    def _():
        relay(last)
        first(sdown)

    first(3)
    first(4)
    arrive(wts.at[pl.ds(0, 2), 0, 1 - core], r4.at[0])
    near_over(0)
    near_over(1)
    if staged:
        ffn_loop(low, high, runs_of(near_slots))
    if nz > 3:
        travel(3, 0)
    finish(0)
    finish(1)
    finish(2)
    if nz > 3:
        travel(3, 1)
    for step in range(4, nz):
        for h in range(2):
            travel(step, h)
    diag_over(0)

    def early(i, carry):
        gbuf[pl.ds(i * pack, pack)] = project(0, i * pack, pack, dlo, dhi).reshape(pack, rows, gbuf.shape[2])
        return carry

    if staged:
        ffn_loop(0, low, runs_of(near_slots))
        ffn_loop(high, nz, runs_of(near_slots))
        lax.fori_loop(0, nz // pack, early, 0)
    diag_over(1)

    def late(i, carry):
        p = i * pack
        if staged:
            gate = gbuf[pl.ds(p, pack)].reshape(pack * rows, gbuf.shape[2])
            val = weighted(gate, project(1, p, pack, dlo, dhi), p, pack)
            hid[pl.ds(p, pack), :, dlo * 2 * own_rows : dhi * 2 * own_rows] = val
        else:
            ffn(p, pack, [(0, tp)])
        return carry

    lax.fori_loop(0, nz // pack, late, 0)
    arrive(wts.at[2, 0, 1 - core], r4.at[1])
    near_over(2)
    relay(3)
    first(5)

    @pl.when(shares)
    def _():
        finish(last)
        relay(sdown)
        for n in range(1, SPIECES):
            first(sdown + n)
        arrive(swts.at[pl.ds(0, 2), 0, 1 - core], r4.at[2])
        arrive(swts.at[2, 0, 1 - core], r4.at[3])
        near_over(last)
        diag_over(last)
        sall = 2 * tp * srows

        def shared(i, carry):
            held = act[pl.ds(i * pack, pack)].reshape(pack * rows, d_model)
            gate = lax.dot_general(held, swts[0].reshape(sall, d_model), NT, preferred_element_type=F32)
            up = lax.dot_general(held, swts[1].reshape(sall, d_model), NT, preferred_element_type=F32)
            val = gate * (1.0 / (1.0 + jnp.exp(-gate))) * up
            shid[pl.ds(i * pack, pack)] = val.astype(BF16).reshape(pack, rows, sall)
            return carry

        lax.fori_loop(0, nz // pack, shared, 0)
        finish(sdown)
        near_over(sdown)

    def link(n, d, sign, j):
        cols = pl.ds(n * piece, piece)
        to = nz if (sign < 0 and j == 1) else d
        return remote(ring.at[d, :, cols], ring.at[to, :, cols], sc.at[d], rc.at[n, to], {"ep": e + 2 * sign})

    def landed(n, s):
        arrive(ring.at[s, :, pl.ds(n * piece, piece)], rc.at[n, s])

    def each_link(run):
        for j in range(nz - 1, 0, -1):
            for sign in (1, -1):
                d = z + sign * j
                there = (d < nz) if sign > 0 else (d >= 0)
                depth = z if sign > 0 else nz - 1 - z
                run(d, sign, j, there, depth)

    def send_on(n, lagged):
        lo, hi = n * piece, (n + 1) * piece

        def run(d, sign, j, there, depth):
            @pl.when(there & ((depth >= 2) if lagged else (depth < 2)))
            def _():
                mine_now = acc[n % 2, d]

                @pl.when(depth > 0)
                def _():
                    landed(n, d)
                    ring[d, :, lo:hi] = (mine_now + ring[d, :, lo:hi].astype(F32)).astype(BF16)

                @pl.when(depth == 0)
                def _():
                    ring[d, :, lo:hi] = mine_now.astype(BF16)

                link(n, d, sign, j).start()

        each_link(run)

    starts = {lo: p for p, (lo, count) in enumerate(PIECES)}
    for n in range(CHUNKS):
        lo, hi = n * piece, (n + 1) * piece
        if n in starts:
            p = starts[n]
            if p + 1 < parts:
                finish(2 + p + 1)
            if p + 2 < parts:
                relay(2 + p + 2)
            if p + 4 < parts:
                first(2 + p + 4)
            if p > 0:
                near_over(2 + p)
            diag_over(2 + p)
        q, rest = divmod(n, CHUNKS // SPIECES)
        if rest == 0:

            @pl.when(shares)
            def _():
                if q + 1 < SPIECES:
                    relay(sdown + q + 1)
                if q > 0:
                    finish(sdown + q)
                    near_over(sdown + q)
                diag_over(sdown + q)

        def down(i, carry):
            left = hid[pl.ds(i * pack, pack)].reshape(pack * rows, 2 * tp * own_rows)
            right = wts[2, :, :, :, lo:hi].reshape(2 * tp * own_rows, piece)
            o = jnp.dot(left, right, preferred_element_type=F32)
            acc[n % 2, pl.ds(i * pack, pack)] = o.reshape(pack, rows, piece)

            @pl.when(shares)
            def _():
                more = jnp.dot(
                    shid[pl.ds(i * pack, pack)].reshape(pack * rows, 2 * tp * srows),
                    swts[2, :, :, :, lo:hi].reshape(2 * tp * srows, piece),
                    preferred_element_type=F32,
                )
                acc[n % 2, pl.ds(i * pack, pack)] += more.reshape(pack, rows, piece)

            return carry

        lax.fori_loop(0, nz // pack, down, 0)
        fin[:, lo:hi] = acc[n % 2, z]
        send_on(n, False)
        if n > 0:
            send_on(n - 1, True)
    send_on(CHUNKS - 1, True)

    for n in range(CHUNKS):
        lo, hi = n * piece, (n + 1) * piece

        @pl.when(z > 0)
        def _():
            landed(n, z)
            fin[:, lo:hi] += ring[z, :, lo:hi].astype(F32)

        @pl.when(z < nz - 1)
        def _():
            landed(n, nz)
            fin[:, lo:hi] += ring[nz, :, lo:hi].astype(F32)

        out_ref[:, lo:hi] = fin[:, lo:hi].astype(BF16)

    def left(ref, sem):
        remote(ref, ref, sem, r1.at[0], {"ep": partner}).wait_send()

    for j, count in enumerate((near, ndiag, tp)):
        left(wts.at[:, pl.ds(0, count), core], sx.at[0, j])

        @pl.when(shares)
        def _():
            left(swts.at[:, pl.ds(0, count), core], sx.at[1, j])

    def sent(d, sign, j, there, depth):
        @pl.when(there)
        def _():
            left(ring.at[d], sc.at[d])

    each_link(sent)

    def own_sent(sign, sem):
        left(act.at[z], st.at[sem])
        left(wtab.at[z], sw.at[sem])

    own_tokens(own_sent)
    for step in range(1, nz):
        for sign in (1, -1):
            src = z - sign * step
            there = (src >= 0) if sign > 0 else (src < nz)
            on = (z + 1 < nz) if sign > 0 else (z > 0)

            @pl.when(there & on)
            def _():
                left(act.at[src], st.at[src])
                left(wtab.at[src], sw.at[src])


def body(ep, tp, tokens, norm_gain, expert_ids, gate_weights, eg, eu, ed, sg, su, sd):
    rows, d_model = tokens.shape
    side = math.isqrt(tp)
    xs = side if side * side == tp else tp
    ys = tp // xs
    nz = ep // 2
    own_rows = eg.shape[1]
    nsh = max(1, min(sg.shape[0] // 32, nz - 2))
    srows = sg.shape[0] // (2 * nsh)
    moves = 2 + len(PIECES) + 1 + SPIECES
    dma = pltpu.SemaphoreType.DMA
    vm = pl.BlockSpec(memory_space=pltpu.VMEM)
    hbm = pl.BlockSpec(memory_space=pl.ANY)
    return pl.pallas_call(
        functools.partial(kernel, ep, tp, xs, ys, nsh),
        out_shape=jax.ShapeDtypeStruct((rows, d_model), BF16),
        in_specs=[hbm, vm, vm, vm] + [hbm] * 6,
        out_specs=vm,
        scratch_shapes=[
            pltpu.VMEM((rows, d_model), BF16),
            pltpu.VMEM((nz, rows, d_model), BF16),
            pltpu.VMEM((nz, max(8, ep), rows), F32),
            pltpu.VMEM((nz, rows, max(8, ep)), F32),
            pltpu.VMEM((3, tp, 2, own_rows, d_model), BF16),
            pltpu.VMEM((3, tp, 2, srows, d_model), BF16),
            pltpu.VMEM((nz, rows, 2 * own_rows * (xs - 1) * (ys - 1)) if own_rows % 128 == 0 else (1, 8, 128), F32),
            pltpu.VMEM((nz, rows, 2 * tp * own_rows), BF16),
            pltpu.VMEM((nz, rows, 2 * tp * srows), BF16),
            pltpu.VMEM((2, nz, rows, d_model // CHUNKS), F32),
            pltpu.VMEM((rows, d_model), F32),
            pltpu.VMEM((nz + 1, rows, d_model), BF16),
            dma((7,)),
            dma((2, 3)),
            dma((moves,)),
            dma((moves,)),
            dma((moves, 2)),
            dma((4,)),
            dma((nz + 1,)),
            dma((nz, 2)),
            dma((nz + 1,)),
            dma((nz,)),
            dma((nz,)),
            dma((CHUNKS, nz + 1)),
        ],
        compiler_params=pltpu.CompilerParams(
            collective_id=0, has_side_effects=True, vmem_limit_bytes=62 * 1024 * 1024
        ),
        name="moe",
    )(tokens, norm_gain.reshape(1, d_model), expert_ids.T, gate_weights.T, eg[0], eu[0], ed[0], sg, su, sd)


def solution(mesh):
    in_specs = (
        P(("ep", "tp"), None),
        P(),
        P(("ep", "tp"), None),
        P(("ep", "tp"), None),
        P("ep", "tp", None),
        P("ep", "tp", None),
        P("ep", "tp", None),
        P("tp", None),
        P("tp", None),
        P("tp", None),
    )
    out_specs = P(("ep", "tp"), None)
    return jax.shard_map(
        functools.partial(body, mesh.shape["ep"], mesh.shape["tp"]),
        mesh=mesh, in_specs=in_specs, out_specs=out_specs, check_vma=False,
    )
```

```python
import functools
import math

import jax
import jax.numpy as jnp
from jax import lax
from jax.experimental import pallas as pl
from jax.experimental.pallas import tpu as pltpu
from jax.sharding import PartitionSpec as P

EPS = 1e-06
MESH = pl.DeviceIdType.MESH
NT = (((1,), (1,)), ((), ()))
F32 = jnp.float32
BF16 = jnp.bfloat16
CHUNKS = 8
SPIECES = 2
REACH = 2
HOLD = (2, 1)
PIECES = tuple((n, 1) for n in range(CHUNKS))


def remote(src, dst, send, recv, where):
    return pltpu.make_async_remote_copy(
        src_ref=src, dst_ref=dst, send_sem=send, recv_sem=recv, device_id=where, device_id_type=MESH
    )


def runs_of(slots):
    out = []
    for s in slots:
        if out and out[-1][1] == s:
            out[-1][1] = s + 1
        else:
            out.append([s, s + 1])
    return out


def kernel(
    ep, tp, xs, ys, nsh,
    tok_ref, gain_ref, ids_ref, gw_ref, eg, eu, ed, sg, su, sd, out_ref,
    tokv, act, wtab, wcol, wts, swts, gbuf, hid, shid, acc, fin, ring,
    ld, sx, r1, r2, r3, r4, st, rt, sw, rw, sc, rc,
):
    e = lax.axis_index("ep")
    t = lax.axis_index("tp")
    y, x = t // xs, t % xs
    z, core = e // 2, e % 2
    nz = ep // 2
    partner = e + 1 - 2 * core
    rows, d_model = tok_ref.shape
    own_rows = eg.shape[0]
    srows = swts.shape[3]
    piece = d_model // CHUNKS
    spiece = d_model // SPIECES
    half_rows = rows // 2
    z0 = (nz - nsh) // 2
    parts = len(PIECES)
    last = 2 + parts
    sdown = last + 1
    shares = (z >= z0) & (z < z0 + nsh)

    def at(dy, dx):
        return lax.rem(y + dy, ys) * xs + lax.rem(x + dx, xs)

    def slot(dy, dx):
        return (dy % ys) * xs + dx % xs

    row_off = [(0, i) for i in range(1, xs)]
    col_off = [(i, 0) for i in range(1, ys)]
    near_off = row_off + col_off
    near_slots = sorted([0] + [slot(*o) for o in near_off])
    diag_slots = [s for s in range(tp) if s not in near_slots]
    near, ndiag = len(near_off), len(diag_slots)

    mine = pl.ds(pl.multiple_of(((z - z0) * 2 + core) * srows, srows), srows)
    loads = [
        pltpu.make_async_copy(tok_ref, tokv, ld.at[0]),
        pltpu.make_async_copy(eg, wts.at[0, 0, core], ld.at[1]),
        pltpu.make_async_copy(eu, wts.at[1, 0, core], ld.at[2]),
        pltpu.make_async_copy(ed, wts.at[2, 0, core], ld.at[3]),
    ]
    for c in loads:
        c.start()
    sloads = [pltpu.make_async_copy(r.at[mine], swts.at[i, 0, core], ld.at[4 + i]) for i, r in enumerate((sg, su, sd))]

    @pl.when(shares)
    def _():
        for c in sloads:
            c.start()

    barrier = pltpu.get_barrier_semaphore()
    for o in near_off:
        pl.semaphore_signal(barrier, inc=1, device_id={"tp": at(*o)}, device_id_type=MESH)
    pl.semaphore_signal(barrier, inc=1, device_id={"ep": partner}, device_id_type=MESH)
    for sign in (1, -1):
        on = (z + 1 < nz) if sign > 0 else (z > 0)

        @pl.when(on)
        def _():
            pl.semaphore_signal(barrier, inc=1, device_id={"ep": e + 2 * sign}, device_id_type=MESH)

    chosen = ids_ref.shape[0]
    label = lax.broadcasted_iota(jnp.int32, wtab.shape[1:], 0)
    total = jnp.zeros(wtab.shape[1:], F32)
    for k in range(chosen):
        total = total + jnp.where(ids_ref[k : k + 1, :] == label, gw_ref[k : k + 1, :], 0.0)
    wtab[z] = total

    pl.semaphore_wait(barrier, near + 1 + (z > 0).astype(jnp.int32) + (z < nz - 1).astype(jnp.int32))

    def columns(a):
        if 2 <= a < last:
            lo, count = PIECES[a - 2]
            return lo * piece, count * piece
        if a >= sdown:
            return (a - sdown) * spiece, spiece
        return 0, d_model

    def view(a, s, k, start, size):
        cols = pl.ds(start, size)
        if a < last:
            return wts.at[min(a, 2), s, k, :, cols]
        if a == last:
            return swts.at[pl.ds(0, 2), s, k, :, cols]
        return swts.at[2, s, k, :, cols]

    def block(a, s, k):
        return view(a, s, k, *columns(a))

    def part(a, s, h):
        start, size = columns(a)
        return view(a, s, core, start + h * (size // 2), size // 2)

    def first(a, source=None):
        for dy, dx in near_off:
            to = slot(-dy, -dx)
            remote(block(a, 0, core) if source is None else source, block(a, to, core), sx.at[int(a >= last), 0], r1.at[a], {"tp": at(dy, dx)}).start()

    def second(a):
        for h, (owners, peers) in enumerate(((col_off, row_off), (row_off, col_off))):
            for oy, ox in owners:
                for py, px in peers:
                    to = slot(oy - py, ox - px)
                    remote(part(a, slot(oy, ox), h), part(a, to, h), sx.at[int(a >= last), 1], r2.at[a], {"tp": at(py, px)}).start()

    def over(a, slots, sem):
        for s in slots:
            b = block(a, s, core)
            remote(b, b, sx.at[int(a >= last), 2], sem, {"ep": partner}).start()

    def arrive(ref, sem):
        remote(ref, ref, sx.at[0, 0], sem, {"ep": partner}).wait_recv()

    def relay(a):
        arrive(block(a, pl.ds(0, near), core), r1.at[a])
        second(a)
        over(a, near_slots[1:], r3.at[a, 0])

    def finish(a):
        arrive(block(a, pl.ds(0, ndiag), core), r2.at[a])
        over(a, diag_slots, r3.at[a, 1])

    def near_over(a):
        arrive(block(a, pl.ds(0, near), 1 - core), r3.at[a, 0])

    def diag_over(a):
        arrive(block(a, pl.ds(0, ndiag), 1 - core), r3.at[a, 1])

    def token_copy(src, h, sign, sem):
        ref = act.at[src, pl.ds(h * half_rows, half_rows), :]
        return remote(ref, ref, st.at[sem], rt.at[src, h], {"ep": e + 2 * sign})

    def table_copy(src, sign, sem):
        return remote(wtab.at[src], wtab.at[src], sw.at[sem], rw.at[src], {"ep": e + 2 * sign})

    def travel(step, h):
        for sign in (1, -1):
            src = z - sign * step
            there = (src >= 0) if sign > 0 else (src < nz)
            on = (z + 1 < nz) if sign > 0 else (z > 0)

            @pl.when(there)
            def _():
                if h == 0:
                    table_copy(src, sign, src).wait_recv()
                    wcol[src] = wtab[src].T

                    @pl.when(on)
                    def _():
                        table_copy(src, sign, src).start()

                token_copy(src, h, sign, src).wait_recv()

                @pl.when(on)
                def _():
                    token_copy(src, h, sign, src).start()

    def own_tokens(run):
        for sign in (1, -1):
            on = (z + 1 < nz) if sign > 0 else (z > 0)
            sem = z if sign > 0 else nz

            @pl.when(on)
            def _():
                run(sign, sem)

    first(0, eg)
    loads[0].wait()
    tok = tokv[...].astype(F32)
    nrm = tok * lax.rsqrt(jnp.mean(tok * tok, axis=-1, keepdims=True) + EPS) * gain_ref[...]
    act[z] = nrm.astype(BF16)
    own_tokens(lambda sign, sem: table_copy(z, sign, sem).start())
    for c in loads[1:]:
        c.wait()
    for h in range(2):
        own_tokens(lambda sign, sem: token_copy(z, h, sign, sem).start())
    over(0, [0], r4.at[0])
    over(1, [0], r4.at[0])
    first(1)
    first(2)

    @pl.when(shares)
    def _():
        for c in sloads:
            c.wait()
        first(last)
        first(sdown)
        first(3)
        over(last, [0], r4.at[2])
        own = swts.at[2, 0, core]
        remote(own, own, sx.at[1, 2], r4.at[3], {"ep": partner}).start()

    own = wts.at[2, 0, core]
    remote(own, own, sx.at[0, 2], r4.at[1], {"ep": partner}).start()
    wcol[z] = wtab[z].T

    lanes = lax.broadcasted_iota(jnp.int32, (1, wcol.shape[2]), 1)

    def weighted(gate, up, p, planes):
        m, width = gate.shape
        col = wcol[pl.ds(p, planes)].reshape(m, wcol.shape[2])
        pair = [jnp.sum(jnp.where(lanes == 2 * z + k, col, 0.0), axis=1, keepdims=True) for k in range(2)]
        which = lax.broadcasted_iota(jnp.int32, (1, width), 1) // own_rows % 2
        scale = jnp.where(which == 0, pair[0], pair[1])
        val = gate * (1.0 / (1.0 + jnp.exp(-gate))) * up * scale
        return val.astype(BF16).reshape(planes, rows, width)

    def project(a, p, planes, lo, hi):
        held = act[pl.ds(p, planes)].reshape(planes * rows, d_model)
        weight = wts[a, lo:hi].reshape((hi - lo) * 2 * own_rows, d_model)
        return lax.dot_general(held, weight, NT, preferred_element_type=F32)

    def ffn(p, planes, groups):
        for lo, hi in groups:
            val = weighted(project(0, p, planes, lo, hi), project(1, p, planes, lo, hi), p, planes)
            hid[pl.ds(p, planes), :, lo * 2 * own_rows : hi * 2 * own_rows] = val

    staged = own_rows % 128 == 0 and len(runs_of(near_slots)) == 1
    pack = math.gcd(nz, 4)
    low = jnp.maximum(z - REACH, 0)
    high = jnp.minimum(z + REACH + 1, nz)
    dlo, dhi = min(diag_slots), max(diag_slots) + 1

    for h in range(2):
        travel(1, h)
    relay(0)
    if nz > 2:
        travel(2, 0)
    arrive(wts.at[pl.ds(0, 2), 0, 1 - core], r4.at[0])
    near_over(0)
    if nz > 2:
        travel(2, 1)
    relay(1)
    relay(2)

    @pl.when(jnp.logical_not(shares))
    def _():
        first(3)
        first(4)

    near_over(1)
    groups = runs_of(near_slots)
    pairs = (low + 1) // 2, high // 2
    singles = (low, low + low % 2), (high - high % 2, high)
    beyond = (0, low), (high, nz)

    def early(p, width):
        gbuf[pl.ds(p, width)] = project(0, p, width, dlo, dhi).reshape(width, rows, gbuf.shape[2])

    def planes_loop(span, width, run):
        def step(p, carry):
            run(p * width, width)
            return carry

        lax.fori_loop(*span, step, 0)

    def near_ffn(p, width):
        ffn(p, width, groups)

    if staged:
        planes_loop(pairs, 2, near_ffn)

    @pl.when(shares)
    def _():
        relay(last)
        relay(sdown)
        relay(3)
        first(4)
        first(5)
        for n in range(1, SPIECES):
            first(sdown + n)

    finish(0)
    if staged:
        for span in singles:
            planes_loop(span, 1, near_ffn)
    if nz > 3:
        travel(3, 0)
    diag_over(0)
    if staged:
        planes_loop(pairs, 2, early)
        for span in singles:
            planes_loop(span, 1, early)
    finish(1)
    finish(2)
    if nz > 3:
        travel(3, 1)
    for step in range(4, nz):
        for h in range(2):
            travel(step, h)
    if staged:
        for span in beyond:
            planes_loop(span, 1, near_ffn)

    @pl.when(jnp.logical_not(shares))
    def _():
        relay(3)
        first(5)

    if staged:
        for span in beyond:
            planes_loop(span, 1, early)
    diag_over(1)

    def late(i, carry):
        p = i * pack
        if staged:
            gate = gbuf[pl.ds(p, pack)].reshape(pack * rows, gbuf.shape[2])
            val = weighted(gate, project(1, p, pack, dlo, dhi), p, pack)
            hid[pl.ds(p, pack), :, dlo * 2 * own_rows : dhi * 2 * own_rows] = val
        else:
            ffn(p, pack, [(0, tp)])
        return carry

    lax.fori_loop(0, nz // pack, late, 0)
    arrive(wts.at[2, 0, 1 - core], r4.at[1])
    near_over(2)

    @pl.when(shares)
    def _():
        arrive(swts.at[pl.ds(0, 2), 0, 1 - core], r4.at[2])
        arrive(swts.at[2, 0, 1 - core], r4.at[3])
        near_over(last)
        finish(last)
        finish(sdown)
        diag_over(last)
        sall = 2 * tp * srows

        def shared(i, carry):
            held = act[pl.ds(i * pack, pack)].reshape(pack * rows, d_model)
            gate = lax.dot_general(held, swts[0].reshape(sall, d_model), NT, preferred_element_type=F32)
            up = lax.dot_general(held, swts[1].reshape(sall, d_model), NT, preferred_element_type=F32)
            val = gate * (1.0 / (1.0 + jnp.exp(-gate))) * up
            shid[pl.ds(i * pack, pack)] = val.astype(BF16).reshape(pack, rows, sall)
            return carry

        lax.fori_loop(0, nz // pack, shared, 0)

    def link(n, d, sign, j):
        cols = pl.ds(n * piece, piece)
        to = nz if (sign < 0 and j == 1) else d
        return remote(ring.at[d, :, cols], ring.at[to, :, cols], sc.at[d], rc.at[n, to], {"ep": e + 2 * sign})

    def landed(n, s):
        arrive(ring.at[s, :, pl.ds(n * piece, piece)], rc.at[n, s])

    def each_link(run):
        for j in range(nz - 1, 0, -1):
            for sign in (1, -1):
                d = z + sign * j
                there = (d < nz) if sign > 0 else (d >= 0)
                depth = z if sign > 0 else nz - 1 - z
                run(d, sign, j, there, depth)

    def send_on(n, lagged):
        lo, hi = n * piece, (n + 1) * piece

        def run(d, sign, j, there, depth):
            @pl.when(there & ((depth >= 2) if lagged else (depth < 2)))
            def _():
                mine_now = acc[n % 2, d]

                @pl.when(depth > 0)
                def _():
                    landed(n, d)
                    ring[d, :, lo:hi] = (mine_now + ring[d, :, lo:hi].astype(F32)).astype(BF16)

                @pl.when(depth == 0)
                def _():
                    ring[d, :, lo:hi] = mine_now.astype(BF16)

                if lagged or j > 1:
                    link(n, d, sign, j).start()

        each_link(run)

    def send_late(n, wanted):
        if not 0 <= n < CHUNKS:
            return

        def run(d, sign, j, there, depth):
            if j == 1:

                @pl.when(there & (depth == wanted))
                def _():
                    link(n, d, sign, j).start()

        each_link(run)

    starts = {lo: p for p, (lo, count) in enumerate(PIECES)}
    for n in range(CHUNKS):
        lo, hi = n * piece, (n + 1) * piece
        if n in starts:
            diag_over(2 + starts[n])
        q, rest = divmod(n, CHUNKS // SPIECES)
        if rest == 0:

            @pl.when(shares)
            def _():
                near_over(sdown + q)
                diag_over(sdown + q)

        def down(i, carry):
            left = hid[pl.ds(i * pack, pack)].reshape(pack * rows, 2 * tp * own_rows)
            right = wts[2, :, :, :, lo:hi].reshape(2 * tp * own_rows, piece)
            o = jnp.dot(left, right, preferred_element_type=F32)
            acc[n % 2, pl.ds(i * pack, pack)] = o.reshape(pack, rows, piece)

            @pl.when(shares)
            def _():
                more = jnp.dot(
                    shid[pl.ds(i * pack, pack)].reshape(pack * rows, 2 * tp * srows),
                    swts[2, :, :, :, lo:hi].reshape(2 * tp * srows, piece),
                    preferred_element_type=F32,
                )
                acc[n % 2, pl.ds(i * pack, pack)] += more.reshape(pack, rows, piece)

            return carry

        lax.fori_loop(0, nz // pack, down, 0)
        fin[:, lo:hi] = acc[n % 2, z]
        send_on(n, False)
        send_late(n - HOLD[0], 0)
        send_late(n - HOLD[1], 1)
        if n > 0:
            send_on(n - 1, True)
        if n in starts:
            p = starts[n] + 1
            if p < parts:
                finish(2 + p)
            if p + 1 < parts:
                relay(2 + p + 1)
            for ahead in (p + 3, p + 4) if p == 1 else (p + 4,):
                if ahead < parts:
                    first(2 + ahead)
            if p < parts:
                near_over(2 + p)
        if rest == 1 and q + 1 < SPIECES:

            @pl.when(shares)
            def _():
                relay(sdown + q + 1)

        if rest == CHUNKS // SPIECES - 1 and q + 1 < SPIECES:

            @pl.when(shares)
            def _():
                finish(sdown + q + 1)

    send_on(CHUNKS - 1, True)
    for n in range(CHUNKS, CHUNKS + max(HOLD)):
        send_late(n - HOLD[0], 0)
        send_late(n - HOLD[1], 1)

    for n in range(CHUNKS):
        lo, hi = n * piece, (n + 1) * piece

        @pl.when(z > 0)
        def _():
            landed(n, z)
            fin[:, lo:hi] += ring[z, :, lo:hi].astype(F32)

        @pl.when(z < nz - 1)
        def _():
            landed(n, nz)
            fin[:, lo:hi] += ring[nz, :, lo:hi].astype(F32)

        out_ref[:, lo:hi] = fin[:, lo:hi].astype(BF16)

    def left(ref, sem):
        remote(ref, ref, sem, r1.at[0], {"ep": partner}).wait_send()

    for j, count in enumerate((near, ndiag, tp)):
        left(wts.at[:, pl.ds(0, count), core], sx.at[0, j])

        @pl.when(shares)
        def _():
            left(swts.at[:, pl.ds(0, count), core], sx.at[1, j])

    def sent(d, sign, j, there, depth):
        @pl.when(there)
        def _():
            left(ring.at[d], sc.at[d])

    each_link(sent)

    def own_sent(sign, sem):
        left(act.at[z], st.at[sem])
        left(wtab.at[z], sw.at[sem])

    own_tokens(own_sent)
    for step in range(1, nz):
        for sign in (1, -1):
            src = z - sign * step
            there = (src >= 0) if sign > 0 else (src < nz)
            on = (z + 1 < nz) if sign > 0 else (z > 0)

            @pl.when(there & on)
            def _():
                left(act.at[src], st.at[src])
                left(wtab.at[src], sw.at[src])


def body(ep, tp, tokens, norm_gain, expert_ids, gate_weights, eg, eu, ed, sg, su, sd):
    rows, d_model = tokens.shape
    side = math.isqrt(tp)
    xs = side if side * side == tp else tp
    ys = tp // xs
    nz = ep // 2
    own_rows = eg.shape[1]
    nsh = max(1, min(sg.shape[0] // 32, nz - 2))
    srows = sg.shape[0] // (2 * nsh)
    moves = 2 + len(PIECES) + 1 + SPIECES
    dma = pltpu.SemaphoreType.DMA
    vm = pl.BlockSpec(memory_space=pltpu.VMEM)
    hbm = pl.BlockSpec(memory_space=pl.ANY)
    return pl.pallas_call(
        functools.partial(kernel, ep, tp, xs, ys, nsh),
        out_shape=pltpu.VMEM((rows, d_model), BF16),
        in_specs=[hbm, vm, vm, vm] + [hbm] * 6,
        out_specs=vm,
        scratch_shapes=[
            pltpu.VMEM((rows, d_model), BF16),
            pltpu.VMEM((nz, rows, d_model), BF16),
            pltpu.VMEM((nz, max(8, ep), rows), F32),
            pltpu.VMEM((nz, rows, max(8, ep)), F32),
            pltpu.VMEM((3, tp, 2, own_rows, d_model), BF16),
            pltpu.VMEM((3, tp, 2, srows, d_model), BF16),
            pltpu.VMEM((nz, rows, 2 * own_rows * (xs - 1) * (ys - 1)) if own_rows % 128 == 0 else (1, 8, 128), F32),
            pltpu.VMEM((nz, rows, 2 * tp * own_rows), BF16),
            pltpu.VMEM((nz, rows, 2 * tp * srows), BF16),
            pltpu.VMEM((2, nz, rows, d_model // CHUNKS), F32),
            pltpu.VMEM((rows, d_model), F32),
            pltpu.VMEM((nz + 1, rows, d_model), BF16),
            dma((7,)),
            dma((2, 3)),
            dma((moves,)),
            dma((moves,)),
            dma((moves, 2)),
            dma((4,)),
            dma((nz + 1,)),
            dma((nz, 2)),
            dma((nz + 1,)),
            dma((nz,)),
            dma((nz,)),
            dma((CHUNKS, nz + 1)),
        ],
        compiler_params=pltpu.CompilerParams(
            collective_id=0, has_side_effects=True, vmem_limit_bytes=62 * 1024 * 1024
        ),
        name="moe",
    )(tokens, norm_gain.reshape(1, d_model), expert_ids.T, gate_weights.T, eg[0], eu[0], ed[0], sg, su, sd)


def solution(mesh):
    in_specs = (
        P(("ep", "tp"), None),
        P(),
        P(("ep", "tp"), None),
        P(("ep", "tp"), None),
        P("ep", "tp", None),
        P("ep", "tp", None),
        P("ep", "tp", None),
        P("tp", None),
        P("tp", None),
        P("tp", None),
    )
    out_specs = P(("ep", "tp"), None)
    return jax.shard_map(
        functools.partial(body, mesh.shape["ep"], mesh.shape["tp"]),
        mesh=mesh, in_specs=in_specs, out_specs=out_specs, check_vma=False,
    )
```

```python
import functools
import math

import jax
import jax.numpy as jnp
from jax import lax
from jax.experimental import pallas as pl
from jax.experimental.pallas import tpu as pltpu
from jax.sharding import PartitionSpec as P

EPS = 1e-06
MESH = pl.DeviceIdType.MESH
NT = (((1,), (1,)), ((), ()))
F32 = jnp.float32
BF16 = jnp.bfloat16
CHUNKS = 8
SPIECES = 2
REACH = 2
HOLD = 3
PIECES = tuple((n, 1) for n in range(CHUNKS))


def remote(src, dst, send, recv, where):
    return pltpu.make_async_remote_copy(
        src_ref=src, dst_ref=dst, send_sem=send, recv_sem=recv, device_id=where, device_id_type=MESH
    )


def runs_of(slots):
    out = []
    for s in slots:
        if out and out[-1][1] == s:
            out[-1][1] = s + 1
        else:
            out.append([s, s + 1])
    return out


def kernel(
    ep, tp, xs, ys, nsh,
    tok_ref, gain_ref, ids_ref, gw_ref, eg, eu, ed, sg, su, sd, out_ref,
    tokv, act, wtab, wcol, wts, swts, gbuf, hid, shid, acc, fin, ring,
    ld, sx, r1, r2, r3, r4, st, rt, sw, rw, sc, rc,
):
    e = lax.axis_index("ep")
    t = lax.axis_index("tp")
    y, x = t // xs, t % xs
    z, core = e // 2, e % 2
    nz = ep // 2
    partner = e + 1 - 2 * core
    rows, d_model = tok_ref.shape
    own_rows = eg.shape[0]
    srows = swts.shape[3]
    piece = d_model // CHUNKS
    spiece = d_model // SPIECES
    half_rows = rows // 2
    z0 = (nz - nsh) // 2
    parts = len(PIECES)
    last = 2 + parts
    sdown = last + 1
    shares = (z >= z0) & (z < z0 + nsh)

    def at(dy, dx):
        return lax.rem(y + dy, ys) * xs + lax.rem(x + dx, xs)

    def slot(dy, dx):
        return (dy % ys) * xs + dx % xs

    row_off = [(0, i) for i in range(1, xs)]
    col_off = [(i, 0) for i in range(1, ys)]
    near_off = row_off + col_off
    near_slots = sorted([0] + [slot(*o) for o in near_off])
    diag_slots = [s for s in range(tp) if s not in near_slots]
    near, ndiag = len(near_off), len(diag_slots)

    mine = pl.ds(pl.multiple_of(((z - z0) * 2 + core) * srows, srows), srows)
    loads = [
        pltpu.make_async_copy(tok_ref, tokv, ld.at[0]),
        pltpu.make_async_copy(eg, wts.at[0, 0, core], ld.at[1]),
        pltpu.make_async_copy(eu, wts.at[1, 0, core], ld.at[2]),
        pltpu.make_async_copy(ed, wts.at[2, 0, core], ld.at[3]),
    ]
    for c in loads:
        c.start()
    sloads = [pltpu.make_async_copy(r.at[mine], swts.at[i, 0, core], ld.at[4 + i]) for i, r in enumerate((sg, su, sd))]

    @pl.when(shares)
    def _():
        for c in sloads:
            c.start()

    barrier = pltpu.get_barrier_semaphore()
    for o in near_off:
        pl.semaphore_signal(barrier, inc=1, device_id={"tp": at(*o)}, device_id_type=MESH)
    pl.semaphore_signal(barrier, inc=1, device_id={"ep": partner}, device_id_type=MESH)
    for sign in (1, -1):
        on = (z + 1 < nz) if sign > 0 else (z > 0)

        @pl.when(on)
        def _():
            pl.semaphore_signal(barrier, inc=1, device_id={"ep": e + 2 * sign}, device_id_type=MESH)

    chosen = ids_ref.shape[0]
    label = lax.broadcasted_iota(jnp.int32, wtab.shape[1:], 0)
    total = jnp.zeros(wtab.shape[1:], F32)
    for k in range(chosen):
        total = total + jnp.where(ids_ref[k : k + 1, :] == label, gw_ref[k : k + 1, :], 0.0)
    wtab[z] = total

    pl.semaphore_wait(barrier, near + 1 + (z > 0).astype(jnp.int32) + (z < nz - 1).astype(jnp.int32))

    def columns(a):
        if 2 <= a < last:
            lo, count = PIECES[a - 2]
            return lo * piece, count * piece
        if a >= sdown:
            return (a - sdown) * spiece, spiece
        return 0, d_model

    def view(a, s, k, start, size):
        cols = pl.ds(start, size)
        if a < last:
            return wts.at[min(a, 2), s, k, :, cols]
        if a == last:
            return swts.at[pl.ds(0, 2), s, k, :, cols]
        return swts.at[2, s, k, :, cols]

    def block(a, s, k):
        return view(a, s, k, *columns(a))

    def part(a, s, h):
        start, size = columns(a)
        return view(a, s, core, start + h * (size // 2), size // 2)

    def first(a, source=None):
        for dy, dx in near_off:
            to = slot(-dy, -dx)
            remote(block(a, 0, core) if source is None else source, block(a, to, core), sx.at[int(a >= last), 0], r1.at[a], {"tp": at(dy, dx)}).start()

    def second(a):
        for h, (owners, peers) in enumerate(((col_off, row_off), (row_off, col_off))):
            for oy, ox in owners:
                for py, px in peers:
                    to = slot(oy - py, ox - px)
                    remote(part(a, slot(oy, ox), h), part(a, to, h), sx.at[int(a >= last), 1], r2.at[a], {"tp": at(py, px)}).start()

    def over(a, slots, sem):
        for s in slots:
            b = block(a, s, core)
            remote(b, b, sx.at[int(a >= last), 2], sem, {"ep": partner}).start()

    def arrive(ref, sem):
        remote(ref, ref, sx.at[0, 0], sem, {"ep": partner}).wait_recv()

    def relay(a):
        arrive(block(a, pl.ds(0, near), core), r1.at[a])
        second(a)
        over(a, near_slots[1:], r3.at[a, 0])

    def finish(a):
        arrive(block(a, pl.ds(0, ndiag), core), r2.at[a])
        over(a, diag_slots, r3.at[a, 1])

    def near_over(a):
        arrive(block(a, pl.ds(0, near), 1 - core), r3.at[a, 0])

    def diag_over(a):
        arrive(block(a, pl.ds(0, ndiag), 1 - core), r3.at[a, 1])

    def token_copy(src, h, sign, sem):
        ref = act.at[src, pl.ds(h * half_rows, half_rows), :]
        return remote(ref, ref, st.at[sem], rt.at[src, h], {"ep": e + 2 * sign})

    def table_copy(src, sign, sem):
        return remote(wtab.at[src], wtab.at[src], sw.at[sem], rw.at[src], {"ep": e + 2 * sign})

    def travel(step, h):
        for sign in (1, -1):
            src = z - sign * step
            there = (src >= 0) if sign > 0 else (src < nz)
            on = (z + 1 < nz) if sign > 0 else (z > 0)

            @pl.when(there)
            def _():
                if h == 0:
                    table_copy(src, sign, src).wait_recv()
                    wcol[src] = wtab[src].T

                    @pl.when(on)
                    def _():
                        table_copy(src, sign, src).start()

                token_copy(src, h, sign, src).wait_recv()

                @pl.when(on)
                def _():
                    token_copy(src, h, sign, src).start()

    def own_tokens(run):
        for sign in (1, -1):
            on = (z + 1 < nz) if sign > 0 else (z > 0)
            sem = z if sign > 0 else nz

            @pl.when(on)
            def _():
                run(sign, sem)

    first(0, eg)
    loads[0].wait()
    tok = tokv[...].astype(F32)
    nrm = tok * lax.rsqrt(jnp.mean(tok * tok, axis=-1, keepdims=True) + EPS) * gain_ref[...]
    act[z] = nrm.astype(BF16)
    own_tokens(lambda sign, sem: table_copy(z, sign, sem).start())
    for c in loads[1:]:
        c.wait()
    for h in range(2):
        own_tokens(lambda sign, sem: token_copy(z, h, sign, sem).start())
    over(0, [0], r4.at[0])
    over(1, [0], r4.at[0])
    first(1)
    first(2)

    @pl.when(shares)
    def _():
        for c in sloads:
            c.wait()
        first(last)
        first(sdown)
        first(3)
        over(last, [0], r4.at[2])
        own = swts.at[2, 0, core]
        remote(own, own, sx.at[1, 2], r4.at[3], {"ep": partner}).start()

    own = wts.at[2, 0, core]
    remote(own, own, sx.at[0, 2], r4.at[1], {"ep": partner}).start()
    wcol[z] = wtab[z].T

    lanes = lax.broadcasted_iota(jnp.int32, (1, wcol.shape[2]), 1)

    def weighted(gate, up, p, planes):
        m, width = gate.shape
        col = wcol[pl.ds(p, planes)].reshape(m, wcol.shape[2])
        pair = [jnp.sum(jnp.where(lanes == 2 * z + k, col, 0.0), axis=1, keepdims=True) for k in range(2)]
        which = lax.broadcasted_iota(jnp.int32, (1, width), 1) // own_rows % 2
        scale = jnp.where(which == 0, pair[0], pair[1])
        val = gate * (1.0 / (1.0 + jnp.exp(-gate))) * up * scale
        return val.astype(BF16).reshape(planes, rows, width)

    def project(a, p, planes, lo, hi):
        held = act[pl.ds(p, planes)].reshape(planes * rows, d_model)
        weight = wts[a, lo:hi].reshape((hi - lo) * 2 * own_rows, d_model)
        return lax.dot_general(held, weight, NT, preferred_element_type=F32)

    def ffn(p, planes, groups):
        for lo, hi in groups:
            val = weighted(project(0, p, planes, lo, hi), project(1, p, planes, lo, hi), p, planes)
            hid[pl.ds(p, planes), :, lo * 2 * own_rows : hi * 2 * own_rows] = val

    staged = own_rows % 128 == 0 and len(runs_of(near_slots)) == 1
    pack = math.gcd(nz, 4)
    reach = REACH if staged else nz
    low = jnp.maximum(z - reach, 0)
    high = jnp.minimum(z + reach + 1, nz)
    dlo, dhi = min(diag_slots), max(diag_slots) + 1

    for h in range(2):
        travel(1, h)
    relay(0)
    if nz > 2:
        travel(2, 0)
    arrive(wts.at[pl.ds(0, 2), 0, 1 - core], r4.at[0])
    near_over(0)
    if nz > 2:
        travel(2, 1)
    relay(1)
    relay(2)

    @pl.when(jnp.logical_not(shares))
    def _():
        first(3)
        first(4)

    near_over(1)
    groups = runs_of(near_slots)
    pairs = (low + 1) // 2, high // 2
    singles = (low, low + low % 2), (high - high % 2, high)
    beyond = (0, low), (high, nz)

    def early(p, width):
        gbuf[pl.ds(p, width)] = project(0, p, width, dlo, dhi).reshape(width, rows, gbuf.shape[2])

    def planes_loop(span, width, run):
        def step(p, carry):
            run(p * width, width)
            return carry

        lax.fori_loop(*span, step, 0)

    def within(run):
        planes_loop(pairs, 2, run)
        for span in singles:
            planes_loop(span, 1, run)

    def outside(run):
        for span in beyond:
            planes_loop(span, 1, run)

    def near_ffn(p, width):
        ffn(p, width, groups)

    if staged:
        planes_loop(pairs, 2, near_ffn)

    @pl.when(shares)
    def _():
        relay(last)
        relay(sdown)
        relay(3)
        first(4)
        first(5)
        for n in range(1, SPIECES):
            first(sdown + n)
        first(6)

    finish(0)
    if staged:
        for span in singles:
            planes_loop(span, 1, near_ffn)
    if nz > 3:
        travel(3, 0)
    diag_over(0)
    if staged:
        within(early)
    finish(1)
    finish(2)
    if nz > 3:
        travel(3, 1)
    for step in range(4, nz):
        for h in range(2):
            travel(step, h)
    @pl.when(jnp.logical_not(shares))
    def _():
        relay(3)
        first(5)
        first(6)

    diag_over(1)

    def late(p, width):
        if staged:
            gate = gbuf[pl.ds(p, width)].reshape(width * rows, gbuf.shape[2])
            val = weighted(gate, project(1, p, width, dlo, dhi), p, width)
            hid[pl.ds(p, width), :, dlo * 2 * own_rows : dhi * 2 * own_rows] = val
        else:
            ffn(p, width, [(0, tp)])

    within(late)
    arrive(wts.at[2, 0, 1 - core], r4.at[1])
    near_over(2)

    @pl.when(shares)
    def _():
        arrive(swts.at[pl.ds(0, 2), 0, 1 - core], r4.at[2])
        arrive(swts.at[2, 0, 1 - core], r4.at[3])
        near_over(last)
        finish(last)
        finish(sdown)
        diag_over(last)
        sall = 2 * tp * srows

        def shared(i, carry):
            held = act[pl.ds(i * pack, pack)].reshape(pack * rows, d_model)
            gate = lax.dot_general(held, swts[0].reshape(sall, d_model), NT, preferred_element_type=F32)
            up = lax.dot_general(held, swts[1].reshape(sall, d_model), NT, preferred_element_type=F32)
            val = gate * (1.0 / (1.0 + jnp.exp(-gate))) * up
            shid[pl.ds(i * pack, pack)] = val.astype(BF16).reshape(pack, rows, sall)
            return carry

        lax.fori_loop(0, nz // pack, shared, 0)
        relay(4)

    def link(n, d, sign, j):
        cols = pl.ds(n * piece, piece)
        to = nz if (sign < 0 and j == 1) else d
        return remote(ring.at[d, :, cols], ring.at[to, :, cols], sc.at[d], rc.at[n, to], {"ep": e + 2 * sign})

    def landed(n, s):
        arrive(ring.at[s, :, pl.ds(n * piece, piece)], rc.at[n, s])

    def each_link(run):
        for j in range(nz - 1, 0, -1):
            for sign in (-1, 1):
                d = z + sign * j
                there = (d < nz) if sign > 0 else (d >= 0)
                depth = z if sign > 0 else nz - 1 - z
                run(d, sign, j, there, depth)

    def send_on(n, lagged, far=None):
        lo, hi = n * piece, (n + 1) * piece

        def run(d, sign, j, there, depth):
            if far is not None and far != (j > reach):
                return

            waits = (depth >= 1) if j == 1 else (depth >= 2)

            @pl.when(there & (waits if lagged else jnp.logical_not(waits)))
            def _():
                mine_now = acc[n % 2, d]

                @pl.when(depth > 0)
                def _():
                    landed(n, d)
                    ring[d, :, lo:hi] = (mine_now + ring[d, :, lo:hi].astype(F32)).astype(BF16)

                @pl.when(depth == 0)
                def _():
                    ring[d, :, lo:hi] = mine_now.astype(BF16)

                if lagged or j > 1 or n == 0:
                    link(n, d, sign, j).start()

        each_link(run)

    def send_late(n):
        if not 0 < n < CHUNKS:
            return

        def run(d, sign, j, there, depth):
            if j == 1:

                @pl.when(there & (depth == 0))
                def _():
                    link(n, d, sign, j).start()

        each_link(run)

    starts = {lo: p for p, (lo, count) in enumerate(PIECES)}
    for n in range(CHUNKS):
        lo, hi = n * piece, (n + 1) * piece
        if n in starts:
            diag_over(2 + starts[n])
        q, rest = divmod(n, CHUNKS // SPIECES)
        if rest == 0:

            @pl.when(shares)
            def _():
                near_over(sdown + q)
                diag_over(sdown + q)

        def down(p, width):
            left = hid[pl.ds(p, width)].reshape(width * rows, 2 * tp * own_rows)
            right = wts[2, :, :, :, lo:hi].reshape(2 * tp * own_rows, piece)
            o = jnp.dot(left, right, preferred_element_type=F32)
            acc[n % 2, pl.ds(p, width)] = o.reshape(width, rows, piece)

            @pl.when(shares)
            def _():
                more = jnp.dot(
                    shid[pl.ds(p, width)].reshape(width * rows, 2 * tp * srows),
                    swts[2, :, :, :, lo:hi].reshape(2 * tp * srows, piece),
                    preferred_element_type=F32,
                )
                acc[n % 2, pl.ds(p, width)] += more.reshape(width, rows, piece)

        if n == 0 and staged:
            within(down)
            fin[:, lo:hi] = acc[n % 2, z]
            send_on(n, False, False)

            @pl.when(jnp.logical_not(shares))
            def _():
                outside(near_ffn)
                relay(4)

            outside(early)
            outside(late)
            outside(down)
            send_on(n, False, True)
        else:
            if n == 0:

                @pl.when(jnp.logical_not(shares))
                def _():
                    relay(4)

            planes_loop((0, nz // pack), pack, down)
            fin[:, lo:hi] = acc[n % 2, z]
            send_on(n, False)
        send_late(n - HOLD)
        if n > 0:
            send_on(n - 1, True)
        if n in starts:
            p = starts[n] + 1
            if p < parts:
                finish(2 + p)
            if p + 2 < parts:
                relay(2 + p + 2)
            for ahead in (p + 4, p + 5) if p == 1 else (p + 5,):
                if ahead < parts:
                    first(2 + ahead)
            if p < parts:
                near_over(2 + p)
        if rest == 1 and q + 1 < SPIECES:

            @pl.when(shares)
            def _():
                relay(sdown + q + 1)

        if rest == CHUNKS // SPIECES - 1 and q + 1 < SPIECES:

            @pl.when(shares)
            def _():
                finish(sdown + q + 1)

    send_on(CHUNKS - 1, True)
    for n in range(CHUNKS, CHUNKS + HOLD):
        send_late(n - HOLD)

    for n in range(CHUNKS):
        lo, hi = n * piece, (n + 1) * piece

        @pl.when(z > 0)
        def _():
            landed(n, z)
            fin[:, lo:hi] += ring[z, :, lo:hi].astype(F32)

        @pl.when(z < nz - 1)
        def _():
            landed(n, nz)
            fin[:, lo:hi] += ring[nz, :, lo:hi].astype(F32)

        out_ref[:, lo:hi] = fin[:, lo:hi].astype(BF16)

    def left(ref, sem):
        remote(ref, ref, sem, r1.at[0], {"ep": partner}).wait_send()

    for j, count in enumerate((near, ndiag, tp)):
        left(wts.at[:, pl.ds(0, count), core], sx.at[0, j])

        @pl.when(shares)
        def _():
            left(swts.at[:, pl.ds(0, count), core], sx.at[1, j])

    def sent(d, sign, j, there, depth):
        @pl.when(there)
        def _():
            left(ring.at[d], sc.at[d])

    each_link(sent)

    def own_sent(sign, sem):
        left(act.at[z], st.at[sem])
        left(wtab.at[z], sw.at[sem])

    own_tokens(own_sent)
    for step in range(1, nz):
        for sign in (1, -1):
            src = z - sign * step
            there = (src >= 0) if sign > 0 else (src < nz)
            on = (z + 1 < nz) if sign > 0 else (z > 0)

            @pl.when(there & on)
            def _():
                left(act.at[src], st.at[src])
                left(wtab.at[src], sw.at[src])


def body(ep, tp, tokens, norm_gain, expert_ids, gate_weights, eg, eu, ed, sg, su, sd):
    rows, d_model = tokens.shape
    side = math.isqrt(tp)
    xs = side if side * side == tp else tp
    ys = tp // xs
    nz = ep // 2
    own_rows = eg.shape[1]
    nsh = max(1, min(sg.shape[0] // 32, nz - 2))
    srows = sg.shape[0] // (2 * nsh)
    moves = 2 + len(PIECES) + 1 + SPIECES
    dma = pltpu.SemaphoreType.DMA
    vm = pl.BlockSpec(memory_space=pltpu.VMEM)
    hbm = pl.BlockSpec(memory_space=pl.ANY)
    return pl.pallas_call(
        functools.partial(kernel, ep, tp, xs, ys, nsh),
        out_shape=pltpu.VMEM((rows, d_model), BF16),
        in_specs=[hbm, vm, vm, vm] + [hbm] * 6,
        out_specs=vm,
        scratch_shapes=[
            pltpu.VMEM((rows, d_model), BF16),
            pltpu.VMEM((nz, rows, d_model), BF16),
            pltpu.VMEM((nz, max(8, ep), rows), F32),
            pltpu.VMEM((nz, rows, max(8, ep)), F32),
            pltpu.VMEM((3, tp, 2, own_rows, d_model), BF16),
            pltpu.VMEM((3, tp, 2, srows, d_model), BF16),
            pltpu.VMEM((nz, rows, 2 * own_rows * (xs - 1) * (ys - 1)) if own_rows % 128 == 0 else (1, 8, 128), F32),
            pltpu.VMEM((nz, rows, 2 * tp * own_rows), BF16),
            pltpu.VMEM((nz, rows, 2 * tp * srows), BF16),
            pltpu.VMEM((2, nz, rows, d_model // CHUNKS), F32),
            pltpu.VMEM((rows, d_model), F32),
            pltpu.VMEM((nz + 1, rows, d_model), BF16),
            dma((7,)),
            dma((2, 3)),
            dma((moves,)),
            dma((moves,)),
            dma((moves, 2)),
            dma((4,)),
            dma((nz + 1,)),
            dma((nz, 2)),
            dma((nz + 1,)),
            dma((nz,)),
            dma((nz,)),
            dma((CHUNKS, nz + 1)),
        ],
        compiler_params=pltpu.CompilerParams(
            collective_id=0, has_side_effects=True, vmem_limit_bytes=62 * 1024 * 1024
        ),
        name="moe",
    )(tokens, norm_gain.reshape(1, d_model), expert_ids.T, gate_weights.T, eg[0], eu[0], ed[0], sg, su, sd)


def solution(mesh):
    in_specs = (
        P(("ep", "tp"), None),
        P(),
        P(("ep", "tp"), None),
        P(("ep", "tp"), None),
        P("ep", "tp", None),
        P("ep", "tp", None),
        P("ep", "tp", None),
        P("tp", None),
        P("tp", None),
        P("tp", None),
    )
    out_specs = P(("ep", "tp"), None)
    return jax.shard_map(
        functools.partial(body, mesh.shape["ep"], mesh.shape["tp"]),
        mesh=mesh, in_specs=in_specs, out_specs=out_specs, check_vma=False,
    )
```
